32 devices in a mesh: sp: 8 (over z, core), tp: 4 (over y, x).
Axes of the slice: x: 2, y: 2, z: 4, core: 2. Of those that a mesh axis runs over, the one named last changes fastest.
Arguments:
- residual_input: bfloat16 [1024, 2048], P(('sp', 'tp')), may hold values from -6 to 6
- mixer_value_input: bfloat16 [1024, 2048], P('sp', 'tp'), may hold values from -6 to 6
- gate_preactivation: bfloat16 [1024, 2048], P('sp', 'tp'), may hold values from -6 to 6
- state_projection_input: bfloat16 [1024, 2, 4, 128], P('sp'), may hold values from -6 to 6
- step_preactivation: bfloat16 [1024, 2, 32], P('sp', None, 'tp'), may hold values from -6 to 6
- spike_log_decay: float32 [1024, 2, 32], P('sp', None, 'tp'), may hold values from -1 to 0
- value_filter_taps: float32 [5, 2048], P(None, 'tp'), may hold values from -2.5 to 2.5
- state_projection_taps: float32 [5, 2, 4, 128], replicated, may hold values from -2.5 to 2.5
- step_size_bias: float32 [2, 32], P(None, 'tp'), may hold values from -0.5 to 0.5
- head_log_decay: float32 [2, 32], P(None, 'tp'), may hold values from -12 to -3
- gated_norm_gain: float32 [2048], P('tp'), may hold values from 0.1 to 1.9
- mixer_output_weight: bfloat16 [2048, 2048], P('tp'), may hold values from -0.125 to 0.125
- feedforward_norm_gain: float32 [2048], replicated, may hold values from 0.1 to 1.9
- routed_expert_index: int32 [1024, 4], P('sp'), may hold values from 0 to 7, all different within a row; in each aligned block of 128 rows (0 to 127, 128 to 255, ...) at most 96 rows name the same one
- routed_expert_weight: float32 [1024, 4], P('sp'), may hold values from 0.2 to 1.2
- routed_gate_weight: bfloat16 [8, 2048, 2048], P('sp', None, 'tp'), may hold values from -0.125 to 0.125
- routed_up_weight: bfloat16 [8, 2048, 2048], P('sp', None, 'tp'), may hold values from -0.125 to 0.125
- routed_down_weight: bfloat16 [8, 2048, 2048], P('sp', 'tp'), may hold values from -0.1875 to 0.1875
- common_gate_weight: bfloat16 [2048, 2048], P(None, 'tp'), may hold values from -0.125 to 0.125
- common_up_weight: bfloat16 [2048, 2048], P(None, 'tp'), may hold values from -0.125 to 0.125
- common_down_weight: bfloat16 [2048, 2048], P('tp'), may hold values from -0.125 to 0.125
Outputs:
- layer_out: bfloat16 [1024, 2048], P(('sp', 'tp'))
The draws below stay inside these ranges and needn't reach their ends.
Inputs may be any that keep to these rules, and one draw needn't show every extreme that they name: `routed_expert_index`: each row names 4 different experts. In the aligned blocks of 128 rows no expert is named by more than 96 rows, and in some block one expert is named by exactly 96.
All inputs are finite; a program needn't handle non-finite values.
Results may differ from the reference program's by a relative error of at most 0.02.
Values may be sent and summed in bfloat16 or wider, within the bound.
No kernel may reach another device: no remote copies, remote signals or barrier semaphores. Data moves between devices by JAX's collectives and lax.ppermute only.
A program may use at most 64 MiB of HBM per device.

```python
import math
import jax
import jax.numpy as jnp
import numpy as np
from jax import lax

D = 2048
HEADS = 32
HD = 64
GROUPS = 4
STATE = 128
CONV = 5
BLK = 128
TOK_DEV = 128
TOP_K = 4
FF_E = 2048
FF_S = 2048
HW = 2048
TOKENS = 1024
EXPERTS = 8
CAP = 96
N_SP = 8
N_TP = 4


def draw_step_preactivation(key, part):
    noise_key, offset_key = jax.random.split(jax.random.fold_in(key, 11))
    noise = jnp.clip(jax.random.normal(noise_key, (TOKENS, 2, HEADS), jnp.float32), -4.0, 4.0)
    offsets = jax.random.uniform(offset_key, (TOKENS // TOK_DEV, 1, 1), jnp.float32, -1.5, 1.5)
    return (noise + jnp.repeat(offsets, TOK_DEV, axis=0)).astype(jnp.bfloat16)


def draw_head_log_decay(key, part):
    pick_key, fast_key, slow_key = jax.random.split(jax.random.fold_in(key, 23), 3)
    fast_heads = jax.random.randint(pick_key, (2, HEADS), 0, 2) == 0
    fast_rate = jax.random.uniform(fast_key, (2, HEADS), jnp.float32, math.log(1.0 / 80.0), math.log(1.0 / 25.0))
    slow_rate = jnp.log(jax.random.uniform(slow_key, (2, HEADS), jnp.float32, 0.1, 0.6) / TOKENS)
    return jnp.where(fast_heads, fast_rate, slow_rate).astype(jnp.float32)


def draw_spike_log_decay(key, part):
    spot_key, value_key = jax.random.split(jax.random.fold_in(key, 37))
    spike_positions = jax.random.randint(spot_key, (2, 2, HEADS), 0, TOKENS)
    decay_levels = jnp.log(jax.random.uniform(value_key, (2, 2, HEADS), jnp.float32, 0.5, 0.8))
    sequence_line = lax.broadcasted_iota(jnp.int32, (TOKENS, 2, HEADS), 0)
    final_result = jnp.zeros((TOKENS, 2, HEADS), jnp.float32)
    for decay_spike in range(2):
        final_result = final_result + jnp.where(sequence_line == spike_positions[decay_spike][None], decay_levels[decay_spike][None], 0.0)
    return final_result


def strengthened(result, own_key, source, target, parts, factor):
    owner, partner = [(jnp.arange(result.shape[axis_at]) // (result.shape[axis_at] // parts)).reshape([-1 if axis == axis_at else 1 for axis in range(result.ndim)]) for axis_at in (source, target)]
    chosen = jax.random.permutation(own_key, parts)[partner]
    strong = (owner == chosen) | (owner == (partner + parts // 2) % parts)
    return jnp.where(strong, factor * result, result)


def steps_of(own_key, dims, pieces, least, high):
    def one(dim, parts):
        heights = jax.random.uniform(jax.random.fold_in(jax.random.fold_in(own_key, 6), dim), (parts,), jnp.float32, least / len(pieces), high / len(pieces))
        return jnp.repeat(jnp.exp(heights), dims[dim] // parts).reshape((-1,) + (1,) * (len(dims) - dim - 1))

    factor_of = one(*pieces[0])
    for cut in pieces[1:]:
        factor_of = factor_of * one(*cut)
    return factor_of


def assign_block(stream_key, own, number, rows, number_of, top, bound, lean):
    sequence = jax.random.permutation(stream_key, number_of)
    crowded, usual = load_shares(number_of, rows * top, bound, lean, True), load_shares(number_of, rows * top, bound, lean, False)
    places = jnp.arange(number_of)

    def named(sizes, rotation):
        used = int((sizes > 0).sum())
        fixed = max(1, used // 4)
        passed = fixed + (places - fixed + rotation * (used - fixed)) % max(1, number_of - fixed)
        return jnp.zeros((number_of,), jnp.int32).at[sequence[jnp.where(places < fixed, places, passed)]].set(jnp.asarray(sizes, jnp.int32))

    sizes = jnp.where(number % 4 == 0, named(crowded, number // 4), named(usual, number - number // 4 - 1))
    mixed = jax.random.permutation(jax.random.fold_in(own, 3), number_of)
    donor, sink = mixed[0:number_of // 2 * 2:2], mixed[1:number_of // 2 * 2:2]
    slack = jnp.minimum(sizes[donor] - 1, bound - sizes[sink]) // 2
    slack = jnp.where((donor == sequence[0]) | (sink == sequence[0]) | (sizes[sink] == 0), 0, jnp.maximum(slack, 0))
    passed = jax.random.randint(jax.random.fold_in(own, 4), (number_of // 2,), 0, 1 << 20) % (slack + 1)
    sizes = sizes.at[donor].add(-passed).at[sink].add(passed)
    members = jnp.searchsorted(jnp.cumsum(sizes), jnp.arange(rows * top), side="right").astype(jnp.int32)
    listing = members.reshape(top, rows).T
    listing = listing[jax.random.permutation(jax.random.fold_in(own, 1), rows)]
    rotation = jax.random.randint(jax.random.fold_in(own, 2), (rows, 1), 0, top)
    return jnp.take_along_axis(listing, (jnp.arange(top)[None, :] + rotation) % top, axis=1)


def load_shares(number_of, total, most, slope, full):
    weights = [(1 << 20) // math.isqrt(standing ** slope) + 1 for standing in range(1, number_of + 1)]
    largest = most if full else min(most, max(-(-total // number_of), total * weights[0] // sum(weights)))
    least = 1 if total - largest >= number_of - 1 else 0
    holding, surplus = [largest] + [least] * (number_of - 1), total - largest - least * (number_of - 1)
    while surplus > 0:
        free = [i for i in range(1, number_of) if holding[i] < largest] or [i for i in range(1, number_of) if holding[i] < most]
        mass, left = sum([weights[i] for i in free]), surplus
        for i in free:
            addition = min(most - holding[i], max(1, left * weights[i] // mass), surplus)
            holding[i] = holding[i] + addition
            surplus = surplus - addition
    return np.array(holding)


def normal_values(key, extent, width, most, cuts=(), kind=jnp.bfloat16):
    values = width * jax.random.normal(key, extent, jnp.float32)
    if cuts:
        values = values * steps_of(key, extent, cuts, -0.22, 0.18)
    return jnp.clip(values, -most, most).astype(kind)


def heavy_noise(rng, extent, scale, bound, cuts, heavy, kind=jnp.bfloat16):
    result = scale * jax.random.normal(rng, extent, jnp.float32)
    if cuts:
        result = result * steps_of(rng, extent, cuts, -0.22, 0.18)
    return jnp.clip(strengthened(result, jax.random.fold_in(rng, 3), *heavy), -bound, bound).astype(kind)


def setup_inputs(seed: int = 0) -> dict:
    splits = jax.random.split(jax.random.key(seed), 22)
    residual_input = normal_values(splits[0], (TOKENS, D), 1.0, 6.0, ((0, 32),))
    mixer_value_input = normal_values(splits[1], (TOKENS, HW), 1.0, 6.0, ((0, 8), (1, 4)))
    gate_preactivation = normal_values(splits[2], (TOKENS, HW), 1.0, 6.0, ((0, 8), (1, 4)))
    state_projection_input = normal_values(splits[3], (TOKENS, 2, GROUPS, STATE), 1.0, 6.0, ((0, 8),))
    step_preactivation = draw_step_preactivation(jax.random.fold_in(splits[21], 71), 0)
    spike_log_decay = draw_spike_log_decay(jax.random.fold_in(splits[21], 71), 0)
    value_filter_taps = normal_values(splits[6], (CONV, HW), CONV ** -0.5, 2.5, ((1, 4),), jnp.float32)
    state_projection_taps = normal_values(splits[7], (CONV, 2, GROUPS, STATE), CONV ** -0.5, 2.5, (), jnp.float32)
    step_size_bias = jnp.clip(jax.random.uniform(splits[8], (2, HEADS), jnp.float32, -0.5, 0.5) * steps_of(splits[8], (2, HEADS), ((1, 4),), -0.4, 0.0), -0.5, 0.5)
    head_log_decay = draw_head_log_decay(jax.random.fold_in(splits[21], 71), 0)
    gated_norm_gain = jnp.clip(1.0 + 0.18 * jax.random.normal(splits[10], (HW,), jnp.float32), 0.1, 1.9)
    mixer_output_weight = normal_values(splits[11], (HW, D), HW ** -0.5, 0.125, ((0, 4),))
    feedforward_norm_gain = jnp.clip(1.0 + 0.18 * jax.random.normal(splits[12], (D,), jnp.float32), 0.1, 1.9)
    routed_expert_index_keys = jax.random.split(jax.random.fold_in(splits[13], 1), TOKENS // TOK_DEV)
    routed_expert_index_turns = jax.random.permutation(jax.random.fold_in(splits[13], 3), TOKENS // TOK_DEV)
    routed_expert_index = jax.vmap(lambda own, number: assign_block(jax.random.fold_in(splits[13], 2), own, number, TOK_DEV, EXPERTS, TOP_K, CAP, 1))(routed_expert_index_keys, routed_expert_index_turns).reshape((TOKENS, TOP_K))
    routed_expert_weight = jnp.clip(0.2 + 1 * jax.random.uniform(splits[14], (TOKENS, TOP_K), jnp.float32) ** steps_of(splits[14], (TOKENS, TOP_K), ((0, 8),), -0.2, 0.2), 0.2, 1.2)
    routed_gate_weight = normal_values(splits[15], (EXPERTS, D, FF_E), D ** -0.5, 0.125, ((0, 8), (2, 4)))
    routed_up_weight = normal_values(splits[16], (EXPERTS, D, FF_E), D ** -0.5, 0.125, ((0, 8), (2, 4)))
    routed_down_weight = heavy_noise(splits[17], (EXPERTS, FF_E, D), FF_E ** -0.5, 0.1875, ((0, 8), (1, 4)), (1, 2, 4, 2.0))
    common_gate_weight = normal_values(splits[18], (D, FF_S), D ** -0.5, 0.125, ((1, 4),))
    common_up_weight = normal_values(splits[19], (D, FF_S), D ** -0.5, 0.125, ((1, 4),))
    common_down_weight = normal_values(splits[20], (FF_S, D), FF_S ** -0.5, 0.125, ((0, 4),))
    return {"residual_input": residual_input, "mixer_value_input": mixer_value_input, "gate_preactivation": gate_preactivation, "state_projection_input": state_projection_input, "step_preactivation": step_preactivation, "spike_log_decay": spike_log_decay, "value_filter_taps": value_filter_taps, "state_projection_taps": state_projection_taps, "step_size_bias": step_size_bias, "head_log_decay": head_log_decay, "gated_norm_gain": gated_norm_gain, "mixer_output_weight": mixer_output_weight, "feedforward_norm_gain": feedforward_norm_gain, "routed_expert_index": routed_expert_index, "routed_expert_weight": routed_expert_weight, "routed_gate_weight": routed_gate_weight, "routed_up_weight": routed_up_weight, "routed_down_weight": routed_down_weight, "common_gate_weight": common_gate_weight, "common_up_weight": common_up_weight, "common_down_weight": common_down_weight}


EPSILON = 1e-06
HIGHEST = lax.Precision.HIGHEST

def rounded(values):
    return lax.optimization_barrier(values.astype(jnp.bfloat16)).astype(jnp.float32)

def block_pass(inputs, decay_logarithm, b_state, c_state, block_len):
    length, groups, per_group, head_dim = inputs.shape
    states = b_state.shape[-1]
    blocks = length // block_len
    inputs = inputs.reshape(blocks, block_len, groups, per_group, head_dim)
    decay_logarithm = decay_logarithm.reshape(blocks, block_len, groups, per_group)
    b_blocks = b_state.reshape(blocks, block_len, groups, states)
    c_blocks = c_state.reshape(blocks, block_len, groups, states)
    within = jnp.cumsum(decay_logarithm, axis=1)
    row_index = lax.broadcasted_iota(jnp.int32, (block_len, block_len), 0)
    col_index = lax.broadcasted_iota(jnp.int32, (block_len, block_len), 1)
    below_mask = (row_index >= col_index)[None, :, :, None, None]
    spread = within[:, :, None] - within[:, None, :]
    weights = jnp.where(below_mask, jnp.exp(jnp.where(below_mask, spread, 0.0)), 0.0)
    scores = jnp.einsum('cign,cjgn->cijg', c_blocks, b_blocks, precision=HIGHEST)
    output = jnp.einsum('cijgr,cjgrp->cigrp', scores[..., None] * weights, inputs, precision=HIGHEST)
    tail_decay = jnp.exp(within[:, -1:] - within)
    block_ends = jnp.einsum('cjgn,cjgrp->cgrpn', b_blocks, inputs * tail_decay[..., None], precision=HIGHEST)
    totals = within[:, -1]

    def carry_step(carried, pair_item):
        block_total, block_end = pair_item
        return (jnp.exp(block_total)[..., None, None] * carried + block_end, carried)
    zero_state = jnp.zeros((groups, per_group, head_dim, states), jnp.float32)
    last_state, starts = lax.scan(carry_step, zero_state, (totals, block_ends))
    output = output + jnp.einsum('cign,cgrpn->cigrp', c_blocks, starts, precision=HIGHEST) * jnp.exp(within)[..., None]
    offsets = jnp.cumsum(totals, axis=0) - totals
    through = (within + offsets[:, None]).reshape(length, groups, per_group)
    return (output.reshape(length, groups, per_group, head_dim), lax.optimization_barrier(jnp.sum(totals, axis=0)), last_state, through)

def slot_table(expert_ids, experts, capacity):
    row_count, top_count = expert_ids.shape
    flat_ids = expert_ids.reshape(-1)
    one_hot = (flat_ids[:, None] == jnp.arange(experts, dtype=jnp.int32)[None, :]).astype(jnp.int32)
    earlier = jnp.cumsum(one_hot, axis=0) - one_hot
    position = lax.optimization_barrier(jnp.sum(earlier * one_hot, axis=1)).astype(jnp.int32)
    owners = (jnp.arange(row_count * top_count, dtype=jnp.int32) // top_count).astype(jnp.int32)
    table = jnp.full((experts * capacity,), row_count, jnp.int32).at[flat_ids * capacity + position].set(owners)
    return (position.reshape(row_count, top_count), table)

def blocked_sum(hidden, down):
    width_slice = down.shape[0] // N_TP

    def add_block(index, total):
        start = (index * width_slice).astype(jnp.int32)
        left = lax.dynamic_slice_in_dim(hidden, start, width_slice, 1)
        right = lax.dynamic_slice_in_dim(down, start, width_slice, 0)
        return total + rounded(jnp.dot(left, right, preferred_element_type=jnp.float32))
    return lax.fori_loop(0, N_TP, add_block, jnp.zeros((hidden.shape[0], down.shape[1]), jnp.float32))

def reference(residual_input, mixer_value_input, gate_preactivation, state_projection_input, step_preactivation, spike_log_decay, value_filter_taps, state_projection_taps, step_size_bias, head_log_decay, gated_norm_gain, mixer_output_weight, feedforward_norm_gain, routed_expert_index, routed_expert_weight, routed_gate_weight, routed_up_weight, routed_down_weight, common_gate_weight, common_up_weight, common_down_weight):
    seq_rows, mixer_cols = mixer_value_input.shape
    head_count = mixer_cols // HD
    groups, states = (state_projection_input.shape[2], state_projection_input.shape[3])
    per_group = head_count // groups
    taps = value_filter_taps.shape[0]
    margin = taps // 2
    joined = jnp.concatenate([mixer_value_input.astype(jnp.float32), state_projection_input.astype(jnp.float32).reshape(seq_rows, 2 * groups * states)], axis=1)
    kernel = jnp.concatenate([value_filter_taps, state_projection_taps.reshape(taps, 2 * groups * states)], axis=1)
    padded = jnp.pad(joined, ((margin, margin), (0, 0)))
    conv_out = jnp.zeros(joined.shape, jnp.float32)
    for offset in range(taps):
        conv_out = conv_out + kernel[offset] * padded[offset:offset + seq_rows]
    active = jax.nn.silu(conv_out)
    mixer_values = active[:, :mixer_cols].reshape(seq_rows, groups, per_group, HD)
    state_parts = active[:, mixer_cols:].reshape(seq_rows, 2, groups, states)
    b_state, c_state = (state_parts[:, 0], state_parts[:, 1])
    discrete_step_size = jax.nn.softplus(step_preactivation.astype(jnp.float32) + step_size_bias)
    decay_logarithm = spike_log_decay - discrete_step_size * jnp.exp(head_log_decay)
    forward_in = mixer_values * discrete_step_size[:, 0].reshape(seq_rows, groups, per_group)[..., None]
    backward_in = mixer_values * discrete_step_size[:, 1].reshape(seq_rows, groups, per_group)[..., None]
    forward_out = block_pass(forward_in, decay_logarithm[:, 0].reshape(seq_rows, groups, per_group), b_state, c_state, BLK)[0]
    backward_out = block_pass(jnp.flip(backward_in, 0), jnp.flip(decay_logarithm[:, 1].reshape(seq_rows, groups, per_group), 0), jnp.flip(b_state, 0), jnp.flip(c_state, 0), BLK)[0]
    scanned = (forward_out + jnp.flip(backward_out, 0)).reshape(seq_rows, mixer_cols)
    gated = (scanned * jax.nn.silu(gate_preactivation.astype(jnp.float32))).reshape(seq_rows, head_count, HD)
    gated = gated * lax.rsqrt(lax.optimization_barrier(jnp.mean(gated * gated, axis=-1, keepdims=True)) + EPSILON)
    mixed = (gated.reshape(seq_rows, mixer_cols) * gated_norm_gain).astype(jnp.bfloat16)
    projected = blocked_sum(mixed, mixer_output_weight)
    residual = (residual_input.astype(jnp.float32) + projected).astype(jnp.bfloat16)
    widened = residual.astype(jnp.float32)
    normed = (widened * lax.rsqrt(lax.optimization_barrier(jnp.mean(widened * widened, axis=-1, keepdims=True)) + EPSILON) * feedforward_norm_gain).astype(jnp.bfloat16)
    model_width = normed.shape[1]
    shared_hidden = (jax.nn.silu(jnp.dot(normed, common_gate_weight, preferred_element_type=jnp.float32)) * jnp.dot(normed, common_up_weight, preferred_element_type=jnp.float32)).astype(jnp.bfloat16)
    shared_out = blocked_sum(shared_hidden, common_down_weight)
    block_rows = seq_rows // N_SP
    experts = routed_gate_weight.shape[0]
    top_count = routed_expert_index.shape[1]
    capacity = 3 * block_rows * top_count // (2 * experts)
    id_blocks = routed_expert_index.reshape(N_SP, block_rows, top_count)
    weight_blocks = routed_expert_weight.reshape(N_SP, block_rows, top_count)

    def block_tables(block_ids, block_weights):
        position, table = slot_table(block_ids, experts, capacity)
        slot_index = block_ids.reshape(-1) * capacity + position.reshape(-1)
        slot_weight = jnp.zeros((experts * capacity,), jnp.float32).at[slot_index].set(block_weights.reshape(-1))
        return (table, slot_weight)
    tables, slot_weights = jax.vmap(block_tables)(id_blocks, weight_blocks)
    offsets = (jnp.arange(N_SP, dtype=jnp.int32) * block_rows)[:, None]
    global_rows = jnp.where(tables < block_rows, tables + offsets, seq_rows).astype(jnp.int32)
    expert_rows = global_rows.reshape(N_SP, experts, capacity).transpose(1, 0, 2).reshape(experts, N_SP * capacity)
    expert_weights = slot_weights.reshape(N_SP, experts, capacity).transpose(1, 0, 2).reshape(experts, N_SP * capacity)
    padded_norm = jnp.concatenate([normed, jnp.zeros((1, model_width), jnp.bfloat16)], axis=0)

    def expert_step(total, pair_item):
        gate_mat, up_mat, down_mat, rows_index, slot_weight = pair_item
        arrived = padded_norm[rows_index]
        hidden = (jax.nn.silu(jnp.dot(arrived, gate_mat, preferred_element_type=jnp.float32)) * jnp.dot(arrived, up_mat, preferred_element_type=jnp.float32)).astype(jnp.bfloat16)
        out_rows = blocked_sum(hidden, down_mat)
        return (total.at[rows_index].add(slot_weight[:, None] * out_rows), None)
    routed, _ = lax.scan(expert_step, jnp.zeros((seq_rows + 1, model_width), jnp.float32), (routed_gate_weight, routed_up_weight, routed_down_weight, expert_rows, expert_weights))
    feed = shared_out + routed[:seq_rows]
    return (widened + feed).astype(jnp.bfloat16)
```

```python
import functools

import jax
import jax.numpy as jnp
from jax import lax
from jax.experimental import pallas as pl
from jax.experimental.pallas import tpu as pltpu
from jax.sharding import PartitionSpec as P

HD = 64
LANES = 128
EPSILON = 1e-06
HIGHEST = lax.Precision.HIGHEST


def swap(values, axis, distance):
    return lax.ppermute(
        values, axis, [(i, i ^ distance) for i in range(lax.axis_size(axis))]
    )


def wide(values):
    return values.astype(jnp.float32)


def silu(values):
    return values / (1.0 + jnp.exp(-values))


def split3(values):
    high = values.astype(jnp.bfloat16)
    rest = values - wide(high)
    middle = rest.astype(jnp.bfloat16)
    low = (rest - wide(middle)).astype(jnp.bfloat16)
    return (high, middle, low)


def by_head(lane, pair, columns, first):
    left = columns[:, first + 2 * pair : first + 2 * pair + 1]
    right = columns[:, first + 2 * pair + 1 : first + 2 * pair + 2]
    return jnp.where(lane < HD, left, right)


def states_kernel(
    heads,
    margin,
    core_ref,
    main_ref,
    low_ref,
    high_ref,
    taps_ref,
    step_ref,
    spike_ref,
    bias_ref,
    rate_ref,
    x_ref,
    b_ref,
    c_ref,
    cum_ref,
    dt_ref,
    reach_ref,
    send_ref,
    keep_ref,
    factor_ref,
    padded,
    fwd,
    bwd,
):
    length, width = main_ref.shape
    cols = x_ref.shape[1]
    states = b_ref.shape[1]
    padded[0:8, :] = jnp.zeros((8, width), jnp.float32)
    padded[8 + length : 16 + length, :] = jnp.zeros((8, width), jnp.float32)
    padded[8 - margin : 8, :] = wide(low_ref[...])
    padded[8 : 8 + length, :] = wide(main_ref[...])
    padded[8 + length : 8 + length + margin, :] = wide(high_ref[...])
    step = step_ref[...] + bias_ref[...]
    step = jnp.maximum(step, 0.0) + jnp.log1p(jnp.exp(-jnp.abs(step)))
    decay = spike_ref[...] - step * jnp.exp(rate_ref[...])
    row = lax.broadcasted_iota(jnp.int32, (length, length), 0)
    col = lax.broadcasted_iota(jnp.int32, (length, length), 1)
    lower = jnp.where(row >= col, 1.0, 0.0)
    sums = jnp.dot(lower, decay, precision=HIGHEST, preferred_element_type=jnp.float32)
    lane = lax.broadcasted_iota(jnp.int32, (length, LANES), 1)
    forward = lane < heads
    cum = jnp.where(forward, sums, sums - decay)
    total = sums[length - 1 : length, :]
    toward = jnp.exp(total - cum)
    within = jnp.exp(cum)
    coefficient = jnp.where(forward, toward, within) * step
    cum_ref[...] = cum
    dt_ref[...] = step
    reach_ref[...] = jnp.where(forward, within, toward)
    whole = jnp.exp(total)

    def active(first, size):
        acc = None
        for tap in range(2 * margin + 1):
            part = (
                taps_ref[tap : tap + 1, first : first + size]
                * padded[8 - margin + tap : 8 - margin + tap + length, first : first + size]
            )
            acc = part if acc is None else acc + part
        return silu(acc)

    b_values = active(cols, states)
    b_ref[...] = b_values.astype(jnp.bfloat16)
    c_ref[...] = active(cols + states, states).astype(jnp.bfloat16)
    b_turned = b_values.T.astype(jnp.bfloat16)
    second = core_ref[0] == 1
    one = lax.broadcasted_iota(jnp.int32, (1, LANES), 1)
    tail = lax.broadcasted_iota(jnp.int32, (16, LANES), 0)
    for pair in range(cols // LANES):
        at = slice(pair * LANES, (pair + 1) * LANES)
        x_values = active(pair * LANES, LANES)
        x_ref[:, at] = x_values.astype(jnp.bfloat16)
        fwd[:, at] = (x_values * by_head(lane, pair, coefficient, 0)).astype(jnp.bfloat16)
        bwd[:, at] = (x_values * by_head(lane, pair, coefficient, heads)).astype(jnp.bfloat16)
        ahead = by_head(one, pair, whole, 0)
        back = by_head(one, pair, whole, heads)
        sent = jnp.where(second, back, ahead)
        high, middle, low = split3(sent)
        rows = jnp.where(tail == 0, wide(high), jnp.where(tail == 1, wide(middle), wide(low)))
        send_ref[states : states + 16, at] = rows.astype(jnp.bfloat16)
        factor_ref[:, at] = jnp.broadcast_to(jnp.where(second, ahead, back), (8, LANES))
    ahead_state = jnp.dot(b_turned, fwd[...], preferred_element_type=jnp.float32)
    back_state = jnp.dot(b_turned, bwd[...], preferred_element_type=jnp.float32)
    send_ref[0:states, :] = jnp.where(second, back_state, ahead_state).astype(jnp.bfloat16)
    keep_ref[...] = jnp.where(second, ahead_state, back_state)


def inside_kernel(heads, x_ref, b_ref, c_ref, cum_ref, dt_ref, y_ref):
    length, cols = x_ref.shape
    scores = lax.dot_general(
        c_ref[...], b_ref[...], (((1,), (1,)), ((), ())), preferred_element_type=jnp.float32
    )
    cum = cum_ref[...]
    cum_turned = cum.T
    dt_turned = dt_ref[...].T
    row = lax.broadcasted_iota(jnp.int32, (length, length), 0)
    col = lax.broadcasted_iota(jnp.int32, (length, length), 1)
    lane = lax.broadcasted_iota(jnp.int32, (length, LANES), 1)
    for pair in range(cols // LANES):
        at = slice(pair * LANES, (pair + 1) * LANES)
        x_pair = x_ref[:, at]
        products = []
        for head in (2 * pair, 2 * pair + 1):
            back = heads + head
            ahead_sum = cum[:, head : head + 1] - cum_turned[head : head + 1, :]
            back_sum = cum_turned[back : back + 1, :] - cum[:, back : back + 1]
            spread = jnp.where(row > col, ahead_sum, jnp.where(row < col, back_sum, 0.0))
            steps = jnp.where(row >= col, dt_turned[head : head + 1, :], 0.0) + jnp.where(
                row <= col, dt_turned[back : back + 1, :], 0.0
            )
            matrix = (scores * jnp.exp(spread) * steps).astype(jnp.bfloat16)
            products.append(jnp.dot(matrix, x_pair, preferred_element_type=jnp.float32))
        y_ref[:, at] = jnp.where(lane < HD, products[0], products[1])


def finish_kernel(
    heads,
    core_ref,
    y_ref,
    c_ref,
    reach_ref,
    near_ref,
    other_ref,
    gate_ref,
    gain_ref,
    weight_ref,
    out_ref,
    mixed,
):
    length, cols = y_ref.shape
    second = core_ref[0] == 1
    near = near_ref[...]
    other = other_ref[...]
    ahead = jnp.dot(
        c_ref[...],
        jnp.where(second, near, other),
        preferred_element_type=jnp.float32,
    )
    back = jnp.dot(
        c_ref[...],
        jnp.where(second, other, near),
        preferred_element_type=jnp.float32,
    )
    reach = reach_ref[...]
    lane = lax.broadcasted_iota(jnp.int32, (length, LANES), 1)
    for pair in range(cols // LANES):
        at = slice(pair * LANES, (pair + 1) * LANES)
        scanned = (
            y_ref[:, at]
            + by_head(lane, pair, reach, 0) * ahead[:, at]
            + by_head(lane, pair, reach, heads) * back[:, at]
        )
        gated = scanned * silu(wide(gate_ref[:, at]))
        square = gated * gated
        left = jnp.sum(jnp.where(lane < HD, square, 0.0), axis=1, keepdims=True)
        right = jnp.sum(jnp.where(lane < HD, 0.0, square), axis=1, keepdims=True)
        mean = jnp.where(lane < HD, left, right) * (1.0 / HD)
        mixed[:, at] = (gated * lax.rsqrt(mean + EPSILON) * gain_ref[:, at]).astype(jnp.bfloat16)
    out_ref[...] = jnp.dot(
        mixed[...], weight_ref[...], preferred_element_type=jnp.float32
    ).astype(jnp.bfloat16)


def local_call(body, outputs, inputs, scratch=(), scalars=0):
    specs = [pl.BlockSpec(memory_space=pltpu.SMEM)] * scalars
    specs = specs + [pl.BlockSpec(memory_space=pltpu.VMEM)] * (len(inputs) - scalars)
    return pl.pallas_call(
        body,
        out_shape=outputs,
        in_specs=specs,
        out_specs=jax.tree.map(lambda _: pl.BlockSpec(memory_space=pltpu.VMEM), outputs),
        scratch_shapes=list(scratch),
    )(*inputs)


def sum_rows(message, states):
    return wide(message[states : states + 1]) + wide(message[states + 1 : states + 2]) + wide(
        message[states + 2 : states + 3]
    )


def mixer(
    mixer_value_input,
    gate_preactivation,
    state_projection_input,
    step_preactivation,
    spike_log_decay,
    value_filter_taps,
    state_projection_taps,
    step_size_bias,
    head_log_decay,
    gated_norm_gain,
    mixer_output_weight,
):
    length, cols = mixer_value_input.shape
    heads = cols // HD
    groups, states = (state_projection_input.shape[2], state_projection_input.shape[3])
    group = lax.axis_index("tp") * heads * groups // (heads * lax.axis_size("tp"))
    taps = value_filter_taps.shape[0]
    margin = taps // 2
    sp_count = lax.axis_size("sp")
    chips = sp_count // 2
    local_bc = lax.dynamic_index_in_dim(state_projection_input, group, 2, keepdims=False)
    local_taps = lax.dynamic_index_in_dim(state_projection_taps, group, 2, keepdims=False)
    joined = jnp.concatenate([mixer_value_input, local_bc.reshape(length, 2 * states)], axis=1)
    kernel = jnp.concatenate([value_filter_taps, local_taps.reshape(taps, 2 * states)], axis=1)
    low = lax.ppermute(joined[length - margin :], "sp", [(i, i + 1) for i in range(sp_count - 1)])
    high = lax.ppermute(joined[:margin], "sp", [(i + 1, i) for i in range(sp_count - 1)])

    def spread(values):
        flat = wide(values).reshape(-1, 2 * heads)
        return jnp.pad(flat, ((0, 0), (0, LANES - 2 * heads)))

    core = (lax.axis_index("sp") % 2).astype(jnp.int32).reshape(1)
    full = jax.ShapeDtypeStruct
    x, b, c, cum, dt, reach, send, keep, factor = local_call(
        functools.partial(states_kernel, heads, margin),
        (
            full((length, cols), jnp.bfloat16),
            full((length, states), jnp.bfloat16),
            full((length, states), jnp.bfloat16),
            full((length, LANES), jnp.float32),
            full((length, LANES), jnp.float32),
            full((length, LANES), jnp.float32),
            full((states + 16, cols), jnp.bfloat16),
            full((states, cols), jnp.float32),
            full((8, cols), jnp.float32),
        ),
        (
            core,
            joined,
            low,
            high,
            kernel,
            spread(step_preactivation),
            spread(spike_log_decay),
            spread(step_size_bias),
            spread(head_log_decay),
        ),
        (
            pltpu.VMEM((length + 16, joined.shape[1]), jnp.float32),
            pltpu.VMEM((length, cols), jnp.bfloat16),
            pltpu.VMEM((length, cols), jnp.bfloat16),
        ),
        scalars=1,
    )
    partner = swap(send, "sp", 1)
    y = local_call(
        functools.partial(inside_kernel, heads),
        full((length, cols), jnp.float32),
        (x, b, c, cum, dt),
    )
    partner_state = wide(partner[:states])
    partner_factor = sum_rows(partner, states)
    own_factor = factor[:1]
    chip_state = (keep + own_factor * partner_state).astype(jnp.bfloat16)
    chip_factor = jnp.concatenate(split3(own_factor * partner_factor), axis=0)
    message = jnp.concatenate(
        [chip_state, chip_factor, jnp.zeros((13, cols), jnp.bfloat16)], axis=0
    )
    incoming = None
    arrived = [
        lax.ppermute(
            message,
            "sp",
            [(2 * z + 1, 2 * (z + k) + 1) for z in range(chips - k)]
            + [(2 * (z + k), 2 * z) for z in range(chips - k)],
        )
        for k in range(1, chips)
    ]
    for part in arrived[::-1]:
        state = wide(part[:states])
        incoming = state if incoming is None else state + sum_rows(part, states) * incoming
    other = swap(incoming.astype(jnp.bfloat16), "sp", 1)
    near = (partner_state + partner_factor * incoming).astype(jnp.bfloat16)
    return local_call(
        functools.partial(finish_kernel, heads),
        full((length, mixer_output_weight.shape[1]), jnp.bfloat16),
        (
            core,
            y,
            c,
            reach,
            near,
            other,
            gate_preactivation,
            gated_norm_gain.reshape(1, cols),
            mixer_output_weight,
        ),
        (pltpu.VMEM((length, cols), jnp.bfloat16),),
        scalars=1,
    )


def slot_table(expert_ids, experts, capacity):
    row_count, top_count = expert_ids.shape
    flat_ids = expert_ids.reshape(-1)
    one_hot = (flat_ids[:, None] == jnp.arange(experts, dtype=jnp.int32)[None, :]).astype(jnp.int32)
    earlier = jnp.cumsum(one_hot, axis=0) - one_hot
    position = jnp.sum(earlier * one_hot, axis=1)
    owners = jnp.arange(row_count * top_count, dtype=jnp.int32) // top_count
    table = (
        jnp.full((experts * capacity,), row_count, jnp.int32)
        .at[flat_ids * capacity + position]
        .set(owners)
    )
    return (position.reshape(row_count, top_count), table)


def dispatch_feed(
    normed,
    routed_expert_index,
    routed_expert_weight,
    routed_gate_weight,
    routed_up_weight,
    routed_down_weight,
    common_gate_weight,
    common_up_weight,
    common_down_weight,
):
    seq_rows = routed_expert_index.shape[0]
    all_rows = lax.all_gather(normed, "tp", axis=0, tiled=True)
    sp_count = lax.axis_size("sp")
    local_experts = routed_gate_weight.shape[0]
    experts = local_experts * sp_count
    top_count = routed_expert_index.shape[1]
    capacity = 3 * seq_rows * top_count // (2 * experts)
    model_width = all_rows.shape[1]
    position, table = slot_table(routed_expert_index, experts, capacity)
    padded_rows = jnp.concatenate([all_rows, jnp.zeros((1, model_width), jnp.bfloat16)], axis=0)
    outgoing = padded_rows[table].reshape(sp_count, local_experts, capacity, model_width)
    arrived = lax.all_to_all(outgoing, "sp", split_axis=0, concat_axis=0, tiled=True)
    gate_part = jnp.einsum(
        "secd,edf->secf", arrived, routed_gate_weight, preferred_element_type=jnp.float32
    )
    up_part = jnp.einsum(
        "secd,edf->secf", arrived, routed_up_weight, preferred_element_type=jnp.float32
    )
    hidden = (jax.nn.silu(gate_part) * up_part).astype(jnp.bfloat16)
    partial_value = lax.optimization_barrier(
        jnp.einsum(
            "secf,efd->secd", hidden, routed_down_weight, preferred_element_type=jnp.float32
        ).astype(jnp.bfloat16)
    ).astype(jnp.float32)
    summed = lax.psum_scatter(
        partial_value.astype(jnp.bfloat16), "tp", scatter_dimension=3, tiled=True
    ).astype(jnp.float32)
    returned = lax.all_to_all(
        summed.astype(jnp.bfloat16), "sp", split_axis=0, concat_axis=0, tiled=True
    ).astype(summed.dtype)
    slot_index = routed_expert_index * capacity + position
    flat_back = returned.reshape(experts * capacity, returned.shape[3])
    chosen = flat_back[slot_index]
    routed = jnp.sum(routed_expert_weight[..., None] * chosen, axis=1)
    routed_part = lax.all_to_all(
        routed.astype(jnp.bfloat16), "tp", split_axis=0, concat_axis=1, tiled=True
    ).astype(routed.dtype)
    picked_rows = all_rows
    gate_part = jnp.dot(picked_rows, common_gate_weight, preferred_element_type=jnp.float32)
    up_part = jnp.dot(picked_rows, common_up_weight, preferred_element_type=jnp.float32)
    hidden = (jax.nn.silu(gate_part) * up_part).astype(jnp.bfloat16)
    shared_part = lax.psum_scatter(
        jnp.dot(hidden, common_down_weight, preferred_element_type=jnp.float32).astype(jnp.bfloat16),
        "tp",
        scatter_dimension=0,
        tiled=True,
    ).astype(jnp.float32)
    feed = shared_part + routed_part
    return feed


def combine_columns(expert_ids, expert_weights, experts):
    numbers = jnp.arange(experts, dtype=jnp.int32)
    dense = jnp.sum(
        jnp.where(expert_ids[..., None] == numbers, expert_weights[..., None], 0.0), axis=1
    )
    high = dense.astype(jnp.bfloat16)
    low = (dense - lax.optimization_barrier(high).astype(jnp.float32)).astype(jnp.bfloat16)
    padding = jnp.zeros((dense.shape[0], -2 * experts % 128), jnp.bfloat16)
    return jnp.concatenate([high, low, padding], axis=1)


def gather_rows(block):
    tp_count = lax.axis_size("tp")
    chips = lax.axis_size("sp") // 2
    rows, width = block.shape
    arrived = [swap(block, "sp", 2 * k) for k in range(1, chips)]
    near = [block] + [swap(block, "tp", t) for t in range(1, tp_count)]
    far = jnp.concatenate(arrived, axis=0)
    far = [far] + [swap(far, "tp", t) for t in range(1, tp_count)]
    half = jnp.concatenate(near + far, axis=0)
    return (half, swap(half, "sp", 1))


def scatter_rows(own, other, shared):
    tp_count = lax.axis_size("tp")
    chips = lax.axis_size("sp") // 2
    width = own.shape[1]
    near_rows = shared.shape[0]
    rows = near_rows // tp_count
    far_rows = rows * (chips - 1)
    half = own + wide(swap(other.astype(jnp.bfloat16), "sp", 1))
    near = (half[:near_rows] + shared).astype(jnp.bfloat16).reshape(tp_count, rows, width)
    far = half[near_rows:].astype(jnp.bfloat16).reshape(tp_count, far_rows, width)
    far_sum = wide(far[0])
    for t in range(1, tp_count):
        far_sum = far_sum + wide(swap(far[t], "tp", t))
    far_sum = far_sum.astype(jnp.bfloat16).reshape(chips - 1, rows, width)
    parts = [swap(near[t], "tp", t) for t in range(1, tp_count)]
    parts = parts + [swap(far_sum[k - 1], "sp", 2 * k) for k in range(1, chips)]
    total = wide(near[0])
    for part in parts:
        total = total + wide(part)
    return total


def on_device(
    residual_input,
    mixer_value_input,
    gate_preactivation,
    state_projection_input,
    step_preactivation,
    spike_log_decay,
    value_filter_taps,
    state_projection_taps,
    step_size_bias,
    head_log_decay,
    gated_norm_gain,
    mixer_output_weight,
    feedforward_norm_gain,
    routed_expert_index,
    routed_expert_weight,
    routed_gate_weight,
    routed_up_weight,
    routed_down_weight,
    common_gate_weight,
    common_up_weight,
    common_down_weight,
):
    tp_count = lax.axis_size("tp")
    tp_index = lax.axis_index("tp")
    seq_rows = mixer_value_input.shape[0]
    model_width = mixer_output_weight.shape[1]
    rows = seq_rows // tp_count
    products = mixer(
        mixer_value_input,
        gate_preactivation,
        state_projection_input,
        step_preactivation,
        spike_log_decay,
        value_filter_taps,
        state_projection_taps,
        step_size_bias,
        head_log_decay,
        gated_norm_gain,
        mixer_output_weight,
    ).reshape(tp_count, rows, model_width)
    projected = wide(lax.dynamic_index_in_dim(products, tp_index, 0, keepdims=False))
    for t in range(1, tp_count):
        projected = projected + wide(
            swap(lax.dynamic_index_in_dim(products, tp_index ^ t, 0, keepdims=False), "tp", t)
        )
    residual = (residual_input.astype(jnp.float32) + projected).astype(jnp.bfloat16)
    widened = residual.astype(jnp.float32)
    normed = (
        widened
        * lax.rsqrt(jnp.mean(widened * widened, axis=-1, keepdims=True) + EPSILON)
        * feedforward_norm_gain
    ).astype(jnp.bfloat16)
    local_experts = routed_gate_weight.shape[0]
    experts = local_experts * lax.axis_size("sp")
    if experts > 2 * routed_expert_index.shape[1]:
        feed = dispatch_feed(
            normed,
            routed_expert_index,
            routed_expert_weight,
            routed_gate_weight,
            routed_up_weight,
            routed_down_weight,
            common_gate_weight,
            common_up_weight,
            common_down_weight,
        )
        return (widened + feed).astype(jnp.bfloat16)
    columns = combine_columns(
        lax.dynamic_slice_in_dim(routed_expert_index, tp_index * rows, rows, 0),
        lax.dynamic_slice_in_dim(routed_expert_weight, tp_index * rows, rows, 0),
        experts,
    )
    own, other = gather_rows(jnp.concatenate([normed, columns], axis=1))
    everyone = jnp.concatenate([own, other], axis=0)
    inputs = everyone[:, :model_width]
    high = wide(everyone[:, model_width : model_width + experts])
    low = wide(everyone[:, model_width + experts : model_width + 2 * experts])
    numbers = jnp.arange(experts, dtype=jnp.int32)
    outputs = None
    for local in range(local_experts):
        number = lax.axis_index("sp") * local_experts + local
        scale = jnp.sum(jnp.where(numbers == number, high + low, 0.0), axis=1, keepdims=True)
        gate_part = jnp.dot(inputs, routed_gate_weight[local], preferred_element_type=jnp.float32)
        up_part = jnp.dot(inputs, routed_up_weight[local], preferred_element_type=jnp.float32)
        hidden = (jax.nn.silu(gate_part) * up_part * scale).astype(jnp.bfloat16)
        part = jnp.dot(hidden, routed_down_weight[local], preferred_element_type=jnp.float32)
        outputs = part if outputs is None else outputs + part
    picked_rows = own[:seq_rows, :model_width]
    gate_part = jnp.dot(picked_rows, common_gate_weight, preferred_element_type=jnp.float32)
    up_part = jnp.dot(picked_rows, common_up_weight, preferred_element_type=jnp.float32)
    hidden = (jax.nn.silu(gate_part) * up_part).astype(jnp.bfloat16)
    shared = jnp.dot(hidden, common_down_weight, preferred_element_type=jnp.float32)
    feed = scatter_rows(outputs[: own.shape[0]], outputs[own.shape[0] :], shared)
    return (widened + feed).astype(jnp.bfloat16)


def solution(mesh):
    return jax.shard_map(
        on_device,
        mesh=mesh,
        in_specs=(
            P(("sp", "tp"), None),
            P("sp", "tp"),
            P("sp", "tp"),
            P("sp", None, None, None),
            P("sp", None, "tp"),
            P("sp", None, "tp"),
            P(None, "tp"),
            P(),
            P(None, "tp"),
            P(None, "tp"),
            P("tp"),
            P("tp", None),
            P(),
            P("sp", None),
            P("sp", None),
            P("sp", None, "tp"),
            P("sp", None, "tp"),
            P("sp", "tp", None),
            P(None, "tp"),
            P(None, "tp"),
            P("tp", None),
        ),
        out_specs=P(("sp", "tp"), None),
        check_vma=False,
    )
```

```python
import functools

import jax
import jax.numpy as jnp
from jax import lax
from jax.experimental import pallas as pl
from jax.experimental.pallas import tpu as pltpu
from jax.sharding import PartitionSpec as P


HD = 64
LANES = 128
EPSILON = 1e-06
HIGHEST = lax.Precision.HIGHEST


def swap(values, axis, distance):
    return lax.ppermute(
        values, axis, [(i, i ^ distance) for i in range(lax.axis_size(axis))]
    )


def wide(values):
    return values.astype(jnp.float32)


def silu(values):
    return values / (1.0 + jnp.exp(-values))


def split3(values):
    high = values.astype(jnp.bfloat16)
    rest = values - wide(high)
    middle = rest.astype(jnp.bfloat16)
    low = (rest - wide(middle)).astype(jnp.bfloat16)
    return (high, middle, low)


def by_head(lane, pair, columns, first):
    left = columns[:, first + 2 * pair : first + 2 * pair + 1]
    right = columns[:, first + 2 * pair + 1 : first + 2 * pair + 2]
    return jnp.where(lane < HD, left, right)


def by_head_row(lane, pair, rows, first):
    left = rows[first + 2 * pair : first + 2 * pair + 1, :]
    right = rows[first + 2 * pair + 1 : first + 2 * pair + 2, :]
    return jnp.where(lane < HD, left, right)


def prepare_kernel(
    heads,
    place_ref,
    project_ref,
    bias_hbm,
    rate_hbm,
    value_hbm,
    value_taps_hbm,
    project_taps_hbm,
    step_hbm,
    spike_hbm,
    conv_ref,
    taps_ref,
    cum_ref,
    cum_row_ref,
    dt_row_ref,
    reach_ref,
    weight_ref,
    whole_ref,
    padded,
    square,
    bias_ref,
    rate_ref,
    value_ref,
    value_taps_ref,
    project_taps_ref,
    step_ref,
    spike_ref,
    done,
):
    copies = [
        pltpu.make_async_copy(source, target, done.at[number])
        for number, (source, target) in enumerate(
            (
                (bias_hbm, bias_ref),
                (rate_hbm, rate_ref),
                (value_hbm, value_ref),
                (value_taps_hbm, value_taps_ref),
                (project_taps_hbm, project_taps_ref),
                (step_hbm, step_ref),
                (spike_hbm, spike_ref),
            )
        )
    ]
    for copy in copies:
        copy.start()
    length, cols = value_ref.shape
    width = conv_ref.shape[1]
    states = (width - cols) // 2
    taps = value_taps_ref.shape[0]
    margin = taps // 2
    padded[0:8, :] = jnp.zeros((8, width), jnp.float32)
    padded[8 + length : 16 + length, :] = jnp.zeros((8, width), jnp.float32)
    for copy in copies:
        copy.wait()
    padded[8 : 8 + length, 0:cols] = wide(value_ref[...])
    padded[8 : 8 + length, cols:width] = wide(project_ref[...])
    group = place_ref[1]
    taps_ref[0:taps, 0:cols] = value_taps_ref[...]
    for tap in range(taps):
        for part in range(2):
            first = cols + part * states
            taps_ref[tap : tap + 1, first : first + states] = project_taps_ref[
                tap, part, pl.ds(group, 1), :
            ]
    for first in range(0, width, LANES):
        at = slice(first, first + LANES)
        acc = None
        for tap in range(taps):
            start = 8 - margin + tap
            part = taps_ref[tap : tap + 1, at] * padded[start : start + length, at]
            acc = part if acc is None else acc + part
        conv_ref[:, at] = acc
    count = 2 * heads
    tall = lax.broadcasted_iota(jnp.int32, (count, length), 0)
    bias = jnp.zeros((count, length), jnp.float32)
    rate = jnp.zeros((count, length), jnp.float32)
    for way in range(2):
        for head in range(heads):
            here = tall == way * heads + head
            bias = jnp.where(here, bias_ref[way : way + 1, head : head + 1], bias)
            rate = jnp.where(here, rate_ref[way : way + 1, head : head + 1], rate)
    step = wide(step_ref[...]) + bias
    step = jnp.maximum(step, 0.0) + jnp.log1p(jnp.exp(-jnp.abs(step)))
    decay = spike_ref[...] - step * jnp.exp(rate)
    row = lax.broadcasted_iota(jnp.int32, (length, length), 0)
    col = lax.broadcasted_iota(jnp.int32, (length, length), 1)
    upper = jnp.where(row <= col, 1.0, 0.0)
    sums = jnp.dot(decay, upper, precision=HIGHEST, preferred_element_type=jnp.float32)
    forward = tall < heads
    cum = jnp.where(forward, sums, sums - decay)
    total = sums[:, length - 1 : length]
    toward = jnp.exp(total - cum)
    within = jnp.exp(cum)
    whole = jnp.exp(total)
    cum_row_ref[...] = cum
    dt_row_ref[...] = step

    def turned(rows):
        square[0:count, :] = rows
        return square[...].T

    square[...] = jnp.zeros((LANES, length), jnp.float32)
    cum_ref[...] = turned(cum)
    reach_ref[...] = turned(jnp.where(forward, within, toward))
    weight_ref[...] = turned(jnp.where(forward, toward, within) * step)
    one = lax.broadcasted_iota(jnp.int32, (1, LANES), 1)
    for pair in range(cols // LANES):
        at = slice(pair * LANES, (pair + 1) * LANES)
        whole_ref[0:1, at] = by_head_row(one, pair, whole, 0)
        whole_ref[1:2, at] = by_head_row(one, pair, whole, heads)


def states_kernel(
    heads,
    margin,
    place_ref,
    conv_ref,
    low_ref,
    high_ref,
    taps_ref,
    weight_ref,
    whole_ref,
    x_ref,
    b_ref,
    c_ref,
    send_ref,
    keep_ref,
    factor_ref,
    full,
    fwd,
    bwd,
):
    length, cols = x_ref.shape
    states = b_ref.shape[1]
    full[...] = conv_ref[...]
    for r in range(margin):
        first = None
        last = None
        for k in range(margin - r):
            part = taps_ref[k : k + 1, :] * wide(low_ref[r + k : r + k + 1, :])
            first = part if first is None else first + part
            tap = 2 * margin - k
            part = taps_ref[tap : tap + 1, :] * wide(
                high_ref[margin - 1 - r - k : margin - r - k, :]
            )
            last = part if last is None else last + part
        full[r : r + 1, :] = full[r : r + 1, :] + first
        full[length - 1 - r : length - r, :] = full[length - 1 - r : length - r, :] + last
    b_values = silu(full[:, cols : cols + states])
    b_ref[...] = b_values.astype(jnp.bfloat16)
    c_ref[...] = silu(full[:, cols + states :]).astype(jnp.bfloat16)
    b_turned = b_values.T.astype(jnp.bfloat16)
    second = place_ref[0] == 1
    lane = lax.broadcasted_iota(jnp.int32, (length, LANES), 1)
    tail = lax.broadcasted_iota(jnp.int32, (16, LANES), 0)
    weights = weight_ref[...]
    for pair in range(cols // LANES):
        at = slice(pair * LANES, (pair + 1) * LANES)
        x_values = silu(full[:, at])
        x_ref[:, at] = x_values.astype(jnp.bfloat16)
        fwd[:, at] = (x_values * by_head(lane, pair, weights, 0)).astype(jnp.bfloat16)
        bwd[:, at] = (x_values * by_head(lane, pair, weights, heads)).astype(jnp.bfloat16)
        ahead = whole_ref[0:1, at]
        back = whole_ref[1:2, at]
        sent = jnp.where(second, back, ahead)
        high, middle, low = split3(sent)
        rows = jnp.where(tail == 0, wide(high), jnp.where(tail == 1, wide(middle), wide(low)))
        send_ref[states : states + 16, at] = rows.astype(jnp.bfloat16)
        factor_ref[:, at] = jnp.broadcast_to(jnp.where(second, ahead, back), (8, LANES))
    ahead_state = jnp.dot(b_turned, fwd[...], preferred_element_type=jnp.float32)
    back_state = jnp.dot(b_turned, bwd[...], preferred_element_type=jnp.float32)
    send_ref[0:states, :] = jnp.where(second, back_state, ahead_state).astype(jnp.bfloat16)
    keep_ref[...] = jnp.where(second, ahead_state, back_state)


def chip_kernel(partner_ref, keep_ref, factor_ref, message_ref):
    states = keep_ref.shape[0]
    own = factor_ref[0:1, :]
    tail = wide(partner_ref[states : states + 16, :])
    factor = own * (tail[0:1] + tail[1:2] + tail[2:3])
    high, middle, low = split3(factor)
    place = lax.broadcasted_iota(jnp.int32, tail.shape, 0)
    rows = jnp.where(place == 0, wide(high), jnp.where(place == 1, wide(middle), wide(low)))
    message_ref[states : states + 16, :] = rows.astype(jnp.bfloat16)
    message_ref[0:states, :] = (keep_ref[...] + own * wide(partner_ref[0:states, :])).astype(
        jnp.bfloat16
    )


def inside_kernel(heads, x_ref, b_ref, c_ref, cum_ref, cum_row_ref, dt_row_ref, y_ref):
    length, cols = x_ref.shape
    scores = lax.dot_general(
        c_ref[...], b_ref[...], (((1,), (1,)), ((), ())), preferred_element_type=jnp.float32
    )
    cum = cum_ref[...]
    cum_turned = cum_row_ref[...]
    dt_turned = dt_row_ref[...]
    row = lax.broadcasted_iota(jnp.int32, (length, length), 0)
    col = lax.broadcasted_iota(jnp.int32, (length, length), 1)
    lane = lax.broadcasted_iota(jnp.int32, (length, LANES), 1)
    for pair in range(cols // LANES):
        at = slice(pair * LANES, (pair + 1) * LANES)
        x_pair = x_ref[:, at]
        products = []
        for head in (2 * pair, 2 * pair + 1):
            back = heads + head
            ahead_sum = cum[:, head : head + 1] - cum_turned[head : head + 1, :]
            back_sum = cum_turned[back : back + 1, :] - cum[:, back : back + 1]
            spread = jnp.where(row > col, ahead_sum, jnp.where(row < col, back_sum, 0.0))
            steps = jnp.where(row >= col, dt_turned[head : head + 1, :], 0.0) + jnp.where(
                row <= col, dt_turned[back : back + 1, :], 0.0
            )
            matrix = (scores * jnp.exp(spread) * steps).astype(jnp.bfloat16)
            products.append(jnp.dot(matrix, x_pair, preferred_element_type=jnp.float32))
        y_ref[:, at] = jnp.where(lane < HD, products[0], products[1])


def finish_kernel(
    heads,
    core_ref,
    y_ref,
    c_ref,
    reach_ref,
    near_ref,
    other_ref,
    gate_ref,
    gain_ref,
    weight_ref,
    *rest,
):
    out_refs, (mixed, moved) = rest[:-2], rest[-2:]
    length, cols = y_ref.shape
    second = core_ref[0] == 1
    near = near_ref[...]
    other = other_ref[...]
    ahead = jnp.dot(
        c_ref[...],
        jnp.where(second, near, other),
        preferred_element_type=jnp.float32,
    )
    back = jnp.dot(
        c_ref[...],
        jnp.where(second, other, near),
        preferred_element_type=jnp.float32,
    )
    reach = reach_ref[...]
    lane = lax.broadcasted_iota(jnp.int32, (length, LANES), 1)
    for pair in range(cols // LANES):
        at = slice(pair * LANES, (pair + 1) * LANES)
        scanned = (
            y_ref[:, at]
            + by_head(lane, pair, reach, 0) * ahead[:, at]
            + by_head(lane, pair, reach, heads) * back[:, at]
        )
        gated = scanned * silu(wide(gate_ref[:, at]))
        square = gated * gated
        left = jnp.sum(jnp.where(lane < HD, square, 0.0), axis=1, keepdims=True)
        right = jnp.sum(jnp.where(lane < HD, 0.0, square), axis=1, keepdims=True)
        mean = jnp.where(lane < HD, left, right) * (1.0 / HD)
        mixed[:, at] = (gated * lax.rsqrt(mean + EPSILON) * gain_ref[:, at]).astype(jnp.bfloat16)
    rows = length // len(out_refs)
    for distance in range(len(out_refs)):
        start = pl.multiple_of((core_ref[2] ^ distance) * rows, rows)
        moved[distance * rows : (distance + 1) * rows, :] = mixed[pl.ds(start, rows), :]
    product = jnp.dot(moved[...], weight_ref[...], preferred_element_type=jnp.float32)
    for distance, out_ref in enumerate(out_refs):
        out_ref[...] = product[distance * rows : (distance + 1) * rows].astype(jnp.bfloat16)


def expert_kernel(number_ref, rows_ref, gate_ref, up_ref, down_ref, out_ref):
    experts, width = gate_ref.shape[0], gate_ref.shape[1]
    total = rows_ref.shape[0]
    tile = min(total, 256)
    for first in range(0, total, tile):
        size = min(tile, total - first)
        inputs = rows_ref[first : first + size, 0:width]
        result = None
        for local in range(experts):
            gate = jnp.dot(inputs, gate_ref[local], preferred_element_type=jnp.float32)
            up = jnp.dot(inputs, up_ref[local], preferred_element_type=jnp.float32)
            hidden = silu(gate) * up
            if rows_ref.shape[1] > width:
                columns = wide(rows_ref[first : first + size, width:])
                lane = lax.broadcasted_iota(jnp.int32, columns.shape, 1)
                number = number_ref[0] + local
                mine = (lane == number) | (lane == number + number_ref[1])
                hidden = hidden * jnp.sum(jnp.where(mine, columns, 0.0), axis=1, keepdims=True)
            part = jnp.dot(
                hidden.astype(jnp.bfloat16), down_ref[local], preferred_element_type=jnp.float32
            )
            result = part if result is None else result + part
        out_ref[first : first + size, :] = result.astype(jnp.bfloat16)


def join_kernel(near_rows, parts, *refs):
    own_ref, back_ref = refs[:2]
    shared_ref = refs[2] if near_rows else None
    out_refs = refs[3:] if near_rows else refs[2:]
    each = len(out_refs) // len(parts)
    rows = own_ref.shape[0] // each
    for index, (first, size) in enumerate(parts):
        for distance in range(each):
            start = distance * rows + first
            out_ref = out_refs[index * each + distance]
            value = wide(own_ref[start : start + size, :]) + wide(
                back_ref[start : start + size, :]
            )
            if near_rows and first == 0:
                more = wide(shared_ref[distance * near_rows : (distance + 1) * near_rows, :])
                out_ref[0:near_rows, :] = (value[:near_rows] + more).astype(jnp.bfloat16)
                if size > near_rows:
                    out_ref[near_rows:size, :] = value[near_rows:].astype(jnp.bfloat16)
            else:
                out_ref[...] = value.astype(jnp.bfloat16)


def local_call(body, outputs, inputs, scratch=(), scalars=0, limit=8, flops=1 << 30, far=0):
    close = len(inputs) - scalars - far
    specs = [pl.BlockSpec(memory_space=pltpu.SMEM)] * scalars
    specs = specs + [pl.BlockSpec(memory_space=pltpu.VMEM)] * close
    specs = specs + [pl.BlockSpec(memory_space=pltpu.HBM)] * far
    return pl.pallas_call(
        body,
        out_shape=outputs,
        in_specs=specs,
        out_specs=jax.tree.map(lambda _: pl.BlockSpec(memory_space=pltpu.VMEM), outputs),
        scratch_shapes=list(scratch),
        compiler_params=pltpu.CompilerParams(vmem_limit_bytes=limit << 20),
        cost_estimate=pl.CostEstimate(
            flops=flops, transcendentals=0, bytes_accessed=1 << 20
        ),
    )(*inputs)


def sum_rows(message, states):
    return (
        wide(message[states : states + 1])
        + wide(message[states + 1 : states + 2])
        + wide(message[states + 2 : states + 3])
    )


def mixer(
    mixer_value_input,
    gate_preactivation,
    state_projection_input,
    step_preactivation,
    spike_log_decay,
    value_filter_taps,
    state_projection_taps,
    step_size_bias,
    head_log_decay,
    gated_norm_gain,
    mixer_output_weight,
):
    length, cols = mixer_value_input.shape
    heads = cols // HD
    groups, states = (state_projection_input.shape[2], state_projection_input.shape[3])
    group = lax.axis_index("tp") * heads * groups // (heads * lax.axis_size("tp"))
    taps = value_filter_taps.shape[0]
    margin = taps // 2
    sp_count = lax.axis_size("sp")
    chips = sp_count // 2
    tp_count = lax.axis_size("tp")
    projections = lax.dynamic_index_in_dim(
        state_projection_input, group, 2, keepdims=False
    ).reshape(length, 2 * states)

    def ends(first, last):
        return jnp.concatenate(
            [mixer_value_input[first:last], projections[first:last]], axis=1
        )

    low = lax.ppermute(
        ends(length - margin, length), "sp", [(i, i + 1) for i in range(sp_count - 1)]
    )
    high = lax.ppermute(ends(0, margin), "sp", [(i + 1, i) for i in range(sp_count - 1)])

    def rows_of(values):
        return jnp.transpose(values, (1, 2, 0)).reshape(2 * heads, length)

    place = jnp.stack(
        [lax.axis_index("sp") % 2, group, lax.axis_index("tp")]
    ).astype(jnp.int32)
    full = jax.ShapeDtypeStruct
    width = cols + 2 * states
    distant = (
        step_size_bias,
        head_log_decay,
        mixer_value_input,
        value_filter_taps,
        state_projection_taps,
        rows_of(step_preactivation),
        rows_of(spike_log_decay),
    )
    distant = [pltpu.with_memory_space_constraint(array, pltpu.HBM) for array in distant]
    conv, all_taps, cum, cum_row, dt_row, reach, weight, whole = local_call(
        functools.partial(prepare_kernel, heads),
        (
            full((length, width), jnp.float32),
            full((8, width), jnp.float32),
            full((length, LANES), jnp.float32),
            full((2 * heads, length), jnp.float32),
            full((2 * heads, length), jnp.float32),
            full((length, LANES), jnp.float32),
            full((length, LANES), jnp.float32),
            full((8, cols), jnp.float32),
        ),
        (place, projections, *distant),
        (
            pltpu.VMEM((length + 16, width), jnp.float32),
            pltpu.VMEM((LANES, length), jnp.float32),
            *[pltpu.VMEM(array.shape, array.dtype) for array in distant],
            pltpu.SemaphoreType.DMA((len(distant),)),
        ),
        scalars=1,
        far=len(distant),
    )
    x, b, c, send, keep, factor = local_call(
        functools.partial(states_kernel, heads, margin),
        (
            full((length, cols), jnp.bfloat16),
            full((length, states), jnp.bfloat16),
            full((length, states), jnp.bfloat16),
            full((states + 16, cols), jnp.bfloat16),
            full((states, cols), jnp.float32),
            full((8, cols), jnp.float32),
        ),
        (place, conv, low, high, all_taps, weight, whole),
        (
            pltpu.VMEM((length, width), jnp.float32),
            pltpu.VMEM((length, cols), jnp.bfloat16),
            pltpu.VMEM((length, cols), jnp.bfloat16),
        ),
        scalars=1,
    )
    partner = swap(send, "sp", 1)
    y = local_call(
        functools.partial(inside_kernel, heads),
        full((length, cols), jnp.float32),
        (x, b, c, cum, cum_row, dt_row),
    )
    partner_state = wide(partner[:states])
    partner_factor = sum_rows(partner, states)
    message = local_call(
        chip_kernel, full(send.shape, jnp.bfloat16), (partner, keep, factor), flops=1 << 20
    )
    incoming = None
    arrived = []
    for k in range(1, chips):
        arrived.append(
            lax.ppermute(
                message,
                "sp",
                [(2 * z + 1, 2 * (z + k) + 1) for z in range(chips - k)]
                + [(2 * (z + k), 2 * z) for z in range(chips - k)],
            )
        )
    for part in arrived[::-1]:
        state = wide(part[:states])
        incoming = state if incoming is None else state + sum_rows(part, states) * incoming
    other = swap(incoming.astype(jnp.bfloat16), "sp", 1)
    near = (partner_state + partner_factor * incoming).astype(jnp.bfloat16)
    return local_call(
        functools.partial(finish_kernel, heads),
        [full((length // tp_count, mixer_output_weight.shape[1]), jnp.bfloat16)] * tp_count,
        (
            place,
            y,
            c,
            reach,
            near,
            other,
            gate_preactivation,
            gated_norm_gain.reshape(1, cols),
            mixer_output_weight,
        ),
        (pltpu.VMEM((length, cols), jnp.bfloat16), pltpu.VMEM((length, cols), jnp.bfloat16)),
        scalars=1,
    )


def slot_table(expert_ids, experts, capacity):
    row_count, top_count = expert_ids.shape
    flat_ids = expert_ids.reshape(-1)
    one_hot = (flat_ids[:, None] == jnp.arange(experts, dtype=jnp.int32)[None, :]).astype(jnp.int32)
    earlier = jnp.cumsum(one_hot, axis=0) - one_hot
    position = jnp.sum(earlier * one_hot, axis=1)
    owners = jnp.arange(row_count * top_count, dtype=jnp.int32) // top_count
    table = (
        jnp.full((experts * capacity,), row_count, jnp.int32)
        .at[flat_ids * capacity + position]
        .set(owners)
    )
    return (position.reshape(row_count, top_count), table)


def dispatch_feed(
    normed,
    routed_expert_index,
    routed_expert_weight,
    routed_gate_weight,
    routed_up_weight,
    routed_down_weight,
    common_gate_weight,
    common_up_weight,
    common_down_weight,
):
    seq_rows = routed_expert_index.shape[0]
    all_rows = lax.all_gather(normed, "tp", axis=0, tiled=True)
    sp_count = lax.axis_size("sp")
    local_experts = routed_gate_weight.shape[0]
    experts = local_experts * sp_count
    top_count = routed_expert_index.shape[1]
    capacity = 3 * seq_rows * top_count // (2 * experts)
    model_width = all_rows.shape[1]
    position, table = slot_table(routed_expert_index, experts, capacity)
    padded_rows = jnp.concatenate([all_rows, jnp.zeros((1, model_width), jnp.bfloat16)], axis=0)
    outgoing = padded_rows[table].reshape(sp_count, local_experts, capacity, model_width)
    arrived = lax.all_to_all(outgoing, "sp", split_axis=0, concat_axis=0, tiled=True)
    gate_part = jnp.einsum(
        "secd,edf->secf", arrived, routed_gate_weight, preferred_element_type=jnp.float32
    )
    up_part = jnp.einsum(
        "secd,edf->secf", arrived, routed_up_weight, preferred_element_type=jnp.float32
    )
    hidden = (jax.nn.silu(gate_part) * up_part).astype(jnp.bfloat16)
    partial_value = lax.optimization_barrier(
        jnp.einsum(
            "secf,efd->secd", hidden, routed_down_weight, preferred_element_type=jnp.float32
        ).astype(jnp.bfloat16)
    ).astype(jnp.float32)
    summed = lax.psum_scatter(
        partial_value.astype(jnp.bfloat16), "tp", scatter_dimension=3, tiled=True
    ).astype(jnp.float32)
    returned = lax.all_to_all(
        summed.astype(jnp.bfloat16), "sp", split_axis=0, concat_axis=0, tiled=True
    ).astype(summed.dtype)
    slot_index = routed_expert_index * capacity + position
    flat_back = returned.reshape(experts * capacity, returned.shape[3])
    chosen = flat_back[slot_index]
    routed = jnp.sum(routed_expert_weight[..., None] * chosen, axis=1)
    routed_part = lax.all_to_all(
        routed.astype(jnp.bfloat16), "tp", split_axis=0, concat_axis=1, tiled=True
    ).astype(routed.dtype)
    picked_rows = all_rows
    gate_part = jnp.dot(picked_rows, common_gate_weight, preferred_element_type=jnp.float32)
    up_part = jnp.dot(picked_rows, common_up_weight, preferred_element_type=jnp.float32)
    hidden = (jax.nn.silu(gate_part) * up_part).astype(jnp.bfloat16)
    shared_part = lax.psum_scatter(
        jnp.dot(hidden, common_down_weight, preferred_element_type=jnp.float32).astype(jnp.bfloat16),
        "tp",
        scatter_dimension=0,
        tiled=True,
    ).astype(jnp.float32)
    feed = shared_part + routed_part
    return feed


def combine_columns(expert_ids, expert_weights, experts):
    numbers = jnp.arange(experts, dtype=jnp.int32)
    dense = jnp.sum(
        jnp.where(expert_ids[..., None] == numbers, expert_weights[..., None], 0.0), axis=1
    )
    high = dense.astype(jnp.bfloat16)
    low = (dense - lax.optimization_barrier(high).astype(jnp.float32)).astype(jnp.bfloat16)
    padding = jnp.zeros((dense.shape[0], -2 * experts % 128), jnp.bfloat16)
    return jnp.concatenate([high, low, padding], axis=1)


def dense_feed(
    block,
    experts,
    routed_gate_weight,
    routed_up_weight,
    routed_down_weight,
    common_gate_weight,
    common_up_weight,
    common_down_weight,
):
    tp_count = lax.axis_size("tp")
    chips = lax.axis_size("sp") // 2
    rows = block.shape[0]
    width = routed_gate_weight.shape[1]
    hidden = routed_gate_weight.shape[2]
    number = jnp.stack(
        [lax.axis_index("sp") * routed_gate_weight.shape[0], experts]
    ).astype(jnp.int32)
    full = jax.ShapeDtypeStruct

    def run(inputs, gate, up, down):
        return local_call(
            expert_kernel,
            full((inputs.shape[0], width), jnp.bfloat16),
            (number, inputs, gate, up, down),
            scalars=1,
            limit=18,
            flops=6 * inputs.shape[0] * width * hidden,
        )

    blocks = [block] + [swap(block, "sp", 2 * k) for k in range(1, chips)]
    pieces = []
    for group in row_groups(chips):
        part = jnp.concatenate([blocks[k] for k in group], axis=0)
        parts = [part] + [swap(part, "tp", t) for t in range(1, tp_count)]
        own = jnp.concatenate(parts, axis=0)
        other = swap(own, "sp", 1)
        near = [values[:rows, :width] for values in parts] if group[0] == 0 else []
        pieces.append((group, own, other, near))
    sums = []
    for group, own, other, near in pieces:
        weights = (routed_gate_weight, routed_up_weight, routed_down_weight)
        extra = []
        if near:
            extra = [
                run(
                    jnp.concatenate(near, axis=0),
                    common_gate_weight[None],
                    common_up_weight[None],
                    common_down_weight[None],
                )
            ]
        back = swap(run(other, *weights), "sp", 1)
        mine = run(own, *weights)
        cuts = [list(range(len(group)))] if near else [[i] for i in range(len(group))][::-1]
        sent = local_call(
            functools.partial(
                join_kernel,
                rows if near else 0,
                [(cut[0] * rows, len(cut) * rows) for cut in cuts],
            ),
            [full((len(cut) * rows, width), jnp.bfloat16) for cut in cuts for _ in range(tp_count)],
            (mine, back, *extra),
            limit=12,
            flops=1 << 24,
        )
        for index, cut in enumerate(cuts):
            values = sent[index * tp_count : (index + 1) * tp_count]
            total = wide(values[0])
            for t in range(1, tp_count):
                total = total + wide(swap(values[t], "tp", t))
            for place, i in enumerate(cut):
                k = group[i]
                value = total[place * rows : (place + 1) * rows]
                if k:
                    value = wide(swap(value.astype(jnp.bfloat16), "sp", 2 * k))
                sums.append(value)
    feed = sums[0]
    for value in sums[1:]:
        feed = feed + value
    return feed


def row_groups(chips):
    split = max(1, chips // 2)
    groups = [list(range(split)), list(range(split, chips))]
    return [group for group in groups if group]


def on_device(
    residual_input,
    mixer_value_input,
    gate_preactivation,
    state_projection_input,
    step_preactivation,
    spike_log_decay,
    value_filter_taps,
    state_projection_taps,
    step_size_bias,
    head_log_decay,
    gated_norm_gain,
    mixer_output_weight,
    feedforward_norm_gain,
    routed_expert_index,
    routed_expert_weight,
    routed_gate_weight,
    routed_up_weight,
    routed_down_weight,
    common_gate_weight,
    common_up_weight,
    common_down_weight,
):
    tp_count = lax.axis_size("tp")
    tp_index = lax.axis_index("tp")
    seq_rows = mixer_value_input.shape[0]
    rows = seq_rows // tp_count
    products = mixer(
        mixer_value_input,
        gate_preactivation,
        state_projection_input,
        step_preactivation,
        spike_log_decay,
        value_filter_taps,
        state_projection_taps,
        step_size_bias,
        head_log_decay,
        gated_norm_gain,
        mixer_output_weight,
    )
    projected = wide(products[0])
    for t in range(1, tp_count):
        projected = projected + wide(swap(products[t], "tp", t))
    residual = (residual_input.astype(jnp.float32) + projected).astype(jnp.bfloat16)
    widened = residual.astype(jnp.float32)
    normed = (
        widened
        * lax.rsqrt(jnp.mean(widened * widened, axis=-1, keepdims=True) + EPSILON)
        * feedforward_norm_gain
    ).astype(jnp.bfloat16)
    local_experts = routed_gate_weight.shape[0]
    experts = local_experts * lax.axis_size("sp")
    if experts > 2 * routed_expert_index.shape[1]:
        feed = dispatch_feed(
            normed,
            routed_expert_index,
            routed_expert_weight,
            routed_gate_weight,
            routed_up_weight,
            routed_down_weight,
            common_gate_weight,
            common_up_weight,
            common_down_weight,
        )
        return (widened + feed).astype(jnp.bfloat16)
    columns = combine_columns(
        lax.dynamic_slice_in_dim(routed_expert_index, tp_index * rows, rows, 0),
        lax.dynamic_slice_in_dim(routed_expert_weight, tp_index * rows, rows, 0),
        experts,
    )
    feed = dense_feed(
        jnp.concatenate([normed, columns], axis=1),
        experts,
        routed_gate_weight,
        routed_up_weight,
        routed_down_weight,
        common_gate_weight,
        common_up_weight,
        common_down_weight,
    )
    return (widened + feed).astype(jnp.bfloat16)


def solution(mesh):
    return jax.shard_map(
        on_device,
        mesh=mesh,
        in_specs=(
            P(("sp", "tp"), None),
            P("sp", "tp"),
            P("sp", "tp"),
            P("sp", None, None, None),
            P("sp", None, "tp"),
            P("sp", None, "tp"),
            P(None, "tp"),
            P(),
            P(None, "tp"),
            P(None, "tp"),
            P("tp"),
            P("tp", None),
            P(),
            P("sp", None),
            P("sp", None),
            P("sp", None, "tp"),
            P("sp", None, "tp"),
            P("sp", "tp", None),
            P(None, "tp"),
            P(None, "tp"),
            P("tp", None),
        ),
        out_specs=P(("sp", "tp"), None),
        check_vma=False,
    )
```
